32 devices in a mesh: sp: 4 (over z), fs: 4 (over y, x), tp: 2 (over core).
Axes of the slice: x: 2, y: 2, z: 4, core: 2. Of those that a mesh axis runs over, the one named last changes fastest.
Arguments:
- tokens: bfloat16 [4, 1024, 2048], P('fs', ('sp', 'tp')), may hold values from -6 to 6
- norm_gain: float32 [2048], replicated, may hold values from 0.1 to 1.9
- w_query: bfloat16 [2048, 1024], P('fs', 'tp'), may hold values from -0.125 to 0.125
- w_key: bfloat16 [2048, 1024], P('fs', 'tp'), may hold values from -0.125 to 0.125
- w_value: bfloat16 [2048, 1024], P('fs', 'tp'), may hold values from -0.125 to 0.125
- w_conv_value: bfloat16 [2048, 1024], P('fs', 'tp'), may hold values from -2 to 2
- w_conv_gate: bfloat16 [2048, 1024], P('fs', 'tp'), may hold values from -0.125 to 0.125
- key_offset: bfloat16 [1024, 16], P('sp', 'tp'), may hold values from -16 to 2
- conv_kernel: float32 [31, 1024], P(None, 'tp'), may hold values from -3 to 3
- conv_gain: float32 [1024], P('tp'), may hold values from 0.1 to 1.9
- w_attn_out: bfloat16 [1024, 2048], P('tp', 'fs'), may hold values from -1 to 1
- w_conv_out: bfloat16 [1024, 2048], P('tp', 'fs'), may hold values from -0.1875 to 0.1875
Outputs:
- mixed: bfloat16 [4, 1024, 2048], P('fs', ('sp', 'tp'))
The draws below stay inside these ranges and needn't reach their ends.
All inputs are finite; a program needn't handle non-finite values.
Results may differ from the reference program's by a relative error of at most 0.0085.
Values may be sent and summed in bfloat16 or wider, within the bound.
No kernel may reach another device: no remote copies, remote signals or barrier semaphores. Data moves between devices by JAX's collectives and lax.ppermute only.
A program may use at most 128 MiB of HBM per device.

```python
import math
import jax
import jax.numpy as jnp
from jax import lax

D = 2048
STICK_HEADS = 16
HD = 64
CC = 1024
KW = 31
TOK_DEV = 256
SBW = 1024
SEQUENCE_LENGTH = 1024
BATCH = 4
N_TP = 2


def draw_key_offset(key, part):
    divisions = jax.random.split(jax.random.fold_in(key, 11), 5)
    base_level = jax.random.uniform(divisions[0], (STICK_HEADS,), jnp.float32, -2.0, 5.0)
    block_shift = jax.random.uniform(divisions[1], (SEQUENCE_LENGTH // TOK_DEV, STICK_HEADS), jnp.float32, -0.8, 0.8)
    block_shift = jnp.repeat(block_shift, TOK_DEV, axis=0)
    roughness = jnp.clip(0.3 * jax.random.normal(divisions[2], (SEQUENCE_LENGTH, STICK_HEADS), jnp.float32), -1.0, 1.0)
    signal_height = base_level[None, :] - math.log(SEQUENCE_LENGTH) + block_shift + roughness
    spike_locations = jax.random.randint(divisions[3], (4,), 0, SEQUENCE_LENGTH)
    spike_flags = jnp.any(jnp.arange(SEQUENCE_LENGTH)[:, None] == spike_locations[None, :], axis=1)
    spike_magnitude = jax.random.uniform(divisions[4], (SEQUENCE_LENGTH, STICK_HEADS), jnp.float32, -1.2, 0.0)
    return jnp.where(spike_flags[:, None], spike_magnitude, signal_height).astype(jnp.bfloat16)


def draw_conv_kernel(key, part):
    divisions = jax.random.split(jax.random.fold_in(key, 23), 2)
    ramp = jnp.exp(jnp.linspace(math.log(0.4), math.log(2.0), CC)).astype(jnp.float32)
    entries = jnp.clip(jax.random.normal(divisions[0], (KW, CC), jnp.float32), -4.0, 4.0)
    common_tap = 0.1
    roughness = jax.random.uniform(divisions[1], (CC,), jnp.float32, 0.5, 1.5)
    return (entries * KW ** (-0.5) * ramp[None, :] * roughness[None, :] + common_tap).astype(jnp.float32)


def draw_w_conv_value(key, part):
    divisions = jax.random.split(jax.random.fold_in(key, 37), 3)
    levels = jnp.exp(jnp.linspace(math.log(0.3), math.log(3.0), CC)).astype(jnp.float32)
    noise = jnp.clip(jax.random.normal(divisions[0], (D, CC), jnp.float32), -4.0, 4.0)
    shared = jnp.clip(jax.random.normal(divisions[1], (D,), jnp.float32), -3.0, 3.0)
    roughness = jax.random.uniform(divisions[2], (CC,), jnp.float32, 0.7, 1.0)
    return ((noise + shared[:, None] * (levels * roughness)[None, :]) * D ** (-0.5)).astype(jnp.bfloat16)


def block_levels(stream_key, shape, pieces, smallest, top_value):
    def one(dim, blocks):
        heights = jax.random.uniform(jax.random.fold_in(jax.random.fold_in(stream_key, 6), dim), (blocks,), jnp.float32, smallest / len(pieces), top_value / len(pieces))
        return jnp.repeat(jnp.exp(heights), shape[dim] // blocks).reshape((-1,) + (1,) * (len(shape) - dim - 1))

    factor_of = one(*pieces[0])
    for cut in pieces[1:]:
        factor_of = factor_of * one(*cut)
    return factor_of


def bell_draw(own_key, extent, scale, limit, pieces=(), kind=jnp.bfloat16):
    gain = block_levels(own_key, extent, pieces, -0.22, 0.18) if pieces else 1.0
    values = jax.random.normal(own_key, extent, jnp.float32) * scale * gain
    return jnp.minimum(jnp.maximum(values, -limit), limit).astype(kind)


def setup_inputs(seed: int = 0) -> dict:
    streams_of = jax.random.split(jax.random.key(seed), 13)
    tokens = bell_draw(streams_of[0], (BATCH, SEQUENCE_LENGTH, D), 1.0, 6.0, ((0, 4), (1, 8)))
    norm_gain = jnp.clip(1.0 + 0.18 * jax.random.normal(streams_of[1], (D,), jnp.float32), 0.1, 1.9)
    w_query = bell_draw(streams_of[2], (D, SBW), D ** -0.5, 0.125, ((0, 4), (1, 2)))
    w_key = bell_draw(streams_of[3], (D, SBW), D ** -0.5, 0.125, ((0, 4), (1, 2)))
    w_value = bell_draw(streams_of[4], (D, SBW), D ** -0.5, 0.125, ((0, 4), (1, 2)))
    w_conv_value = draw_w_conv_value(jax.random.fold_in(streams_of[12], 71), 0)
    w_conv_gate = bell_draw(streams_of[6], (D, CC), D ** -0.5, 0.125, ((0, 4), (1, 2)))
    key_offset = draw_key_offset(jax.random.fold_in(streams_of[12], 71), 0)
    conv_kernel = draw_conv_kernel(jax.random.fold_in(streams_of[12], 71), 0)
    conv_gain = jnp.clip(1.0 + 0.18 * jax.random.normal(streams_of[9], (CC,), jnp.float32), 0.1, 1.9)
    w_attn_out = bell_draw(streams_of[10], (SBW, D), (SBW // 32) ** -0.5, 1.0, ((0, 2), (1, 4)))
    w_conv_out = bell_draw(streams_of[11], (CC, D), CC ** -0.5, 0.1875, ((0, 2), (1, 4)))
    return {"tokens": tokens, "norm_gain": norm_gain, "w_query": w_query, "w_key": w_key, "w_value": w_value, "w_conv_value": w_conv_value, "w_conv_gate": w_conv_gate, "key_offset": key_offset, "conv_kernel": conv_kernel, "conv_gain": conv_gain, "w_attn_out": w_attn_out, "w_conv_out": w_conv_out}


def reference(tokens, norm_gain, w_query, w_key, w_value, w_conv_value, w_conv_gate, key_offset, conv_kernel, conv_gain, w_attn_out, w_conv_out):
    floats = tokens.astype(jnp.float32)
    normed = (floats * lax.rsqrt(lax.optimization_barrier(jnp.mean(floats * floats, axis=2, keepdims=True)) + 1e-06) * norm_gain).astype(jnp.bfloat16)
    flat_rows = normed.reshape(BATCH * SEQUENCE_LENGTH, D)

    def project(weight):
        return jnp.dot(flat_rows, weight, preferred_element_type=jnp.float32).astype(jnp.bfloat16).reshape(BATCH, SEQUENCE_LENGTH, weight.shape[1])
    queries = project(w_query)
    key_rows = project(w_key)
    value_rows = project(w_value)
    conv_value = project(w_conv_value)
    conv_gate = project(w_conv_gate)
    offsets = jnp.transpose(key_offset.astype(jnp.float32))
    key_pos = jnp.arange(SEQUENCE_LENGTH, dtype=jnp.int32)
    blocks = SEQUENCE_LENGTH // TOK_DEV
    score_scale = HD ** (-0.5)

    def one_block(index):
        batch_index = index // blocks
        first_row = index % blocks * TOK_DEV
        seq_query = lax.dynamic_index_in_dim(queries, batch_index, 0, keepdims=False)
        query_block = lax.dynamic_slice_in_dim(seq_query, first_row, TOK_DEV, 0).reshape(TOK_DEV, STICK_HEADS, HD)
        seq_keys = lax.dynamic_index_in_dim(key_rows, batch_index, 0, keepdims=False).reshape(SEQUENCE_LENGTH, STICK_HEADS, HD)
        seq_values = lax.dynamic_index_in_dim(value_rows, batch_index, 0, keepdims=False).reshape(SEQUENCE_LENGTH, STICK_HEADS, HD)
        logits = jnp.einsum('qhd,khd->hqk', query_block.astype(jnp.float32), seq_keys.astype(jnp.float32)) * score_scale
        logits = logits + offsets[:, None, :]
        query_pos = first_row + jnp.arange(TOK_DEV, dtype=jnp.int32)
        allowed = key_pos[None, :] < query_pos[:, None]
        log_keep = jnp.where(allowed[None], jax.nn.log_sigmoid(-logits), 0.0)
        between = lax.cumsum(log_keep, axis=2, reverse=True) - log_keep
        weights = jnp.where(allowed[None], jnp.exp(jax.nn.log_sigmoid(logits) + between), 0.0).astype(jnp.bfloat16)
        result = jnp.einsum('hqk,khd->qhd', weights.astype(jnp.float32), seq_values.astype(jnp.float32))
        return result.reshape(TOK_DEV, SBW).astype(jnp.bfloat16)
    attn_heads = lax.map(one_block, jnp.arange(BATCH * blocks, dtype=jnp.int32)).reshape(BATCH, SEQUENCE_LENGTH, SBW)
    gated_input = (conv_value.astype(jnp.float32) * jax.nn.sigmoid(conv_gate.astype(jnp.float32))).astype(jnp.bfloat16)
    padded = jnp.pad(gated_input, ((0, 0), (KW - 1, 0), (0, 0))).astype(jnp.float32)
    conv_sum = jnp.zeros((BATCH, SEQUENCE_LENGTH, CC), jnp.float32)
    for tap_index in range(KW):
        conv_sum = conv_sum + conv_kernel[tap_index] * padded[:, tap_index:tap_index + SEQUENCE_LENGTH]
    mean_val = lax.optimization_barrier(jnp.mean(conv_sum, axis=2, keepdims=True))
    centred = conv_sum - mean_val
    spread = lax.optimization_barrier(jnp.mean(centred * centred, axis=2, keepdims=True))
    conv_hidden = jax.nn.silu(centred * lax.rsqrt(spread + 1e-06) * conv_gain).astype(jnp.bfloat16)
    head_cols = SBW // N_TP
    chan_cols = CC // N_TP
    attn_flat = attn_heads.reshape(BATCH * SEQUENCE_LENGTH, SBW)
    conv_flat = conv_hidden.reshape(BATCH * SEQUENCE_LENGTH, CC)
    total = jnp.zeros((BATCH * SEQUENCE_LENGTH, D), jnp.float32)
    for group in range(N_TP):
        partial_value = jnp.dot(attn_flat[:, group * head_cols:(group + 1) * head_cols], w_attn_out[group * head_cols:(group + 1) * head_cols], preferred_element_type=jnp.float32)
        partial_value = partial_value + jnp.dot(conv_flat[:, group * chan_cols:(group + 1) * chan_cols], w_conv_out[group * chan_cols:(group + 1) * chan_cols], preferred_element_type=jnp.float32)
        total = total + lax.optimization_barrier(partial_value.astype(jnp.bfloat16)).astype(jnp.float32)
    return total.astype(jnp.bfloat16).reshape(BATCH, SEQUENCE_LENGTH, D)
```

```python
import functools

import jax
import jax.numpy as jnp
from jax import lax
from jax.experimental import pallas as pl
from jax.experimental.pallas import tpu as pltpu
from jax.sharding import PartitionSpec as P

HD = 64
CC = 1024


def shifted(block, axis, distance):
    devices = range(lax.axis_size(axis))
    route = [(i - distance, i) for i in devices if i - distance in devices]
    return lax.ppermute(block, axis, route)


def piece_terms(queries, key_rows, value_rows, offsets, carry_log, allowed):
    head_size = queries.shape[2]
    logits = jnp.einsum(
        "qhd,khd->hqk", queries, key_rows, preferred_element_type=jnp.float32
    ) * head_size ** (-0.5)
    logits = logits + jnp.transpose(offsets.astype(jnp.float32))[:, None, :]
    log_keep = jax.nn.log_sigmoid(-logits)
    if allowed is not None:
        log_keep = jnp.where(allowed[None], log_keep, 0.0)
    between = lax.cumsum(log_keep, axis=2, reverse=True) - log_keep
    weights = jnp.exp(jax.nn.log_sigmoid(logits) + between + carry_log[:, :, None])
    if allowed is not None:
        weights = jnp.where(allowed[None], weights, 0.0)
    result = jnp.einsum(
        "hqk,khd->qhd", weights.astype(jnp.bfloat16), value_rows, preferred_element_type=jnp.float32
    )
    return (result, carry_log + jnp.sum(log_keep, axis=2))


def shards(
    tokens,
    norm_gain,
    w_query,
    w_key,
    w_value,
    w_conv_value,
    w_conv_gate,
    key_offset,
    conv_kernel,
    conv_gain,
    w_attn_out,
    w_conv_out,
):
    gathered = (
        lax.all_gather(w_query, "fs", axis=0, tiled=True),
        lax.all_gather(w_key, "fs", axis=0, tiled=True),
        lax.all_gather(w_value, "fs", axis=0, tiled=True),
        lax.all_gather(w_conv_value, "fs", axis=0, tiled=True),
        lax.all_gather(w_conv_gate, "fs", axis=0, tiled=True),
    )
    floats = lax.all_gather(tokens[0], "tp", axis=0, tiled=True).astype(jnp.float32)
    normed = (
        floats * lax.rsqrt(jnp.mean(floats * floats, axis=1, keepdims=True) + 1e-06) * norm_gain
    ).astype(jnp.bfloat16)
    projected = jnp.concatenate(
        [
            jnp.dot(normed, weight, preferred_element_type=jnp.float32).astype(jnp.bfloat16)
            for weight in gathered
        ],
        axis=1,
    )
    head_cols = w_query.shape[1]
    channels = w_conv_value.shape[1]
    block_len = projected.shape[0]
    local_heads = head_cols // HD
    queries = projected[:, :head_cols].reshape(block_len, local_heads, HD)
    key_flat = projected[:, head_cols : 2 * head_cols]
    value_flat = projected[:, 2 * head_cols : 3 * head_cols]
    conv_value = projected[:, 3 * head_cols : 3 * head_cols + channels]
    conv_gate = projected[:, 3 * head_cols + channels :]
    position = lax.axis_index("sp")
    positions = jnp.arange(block_len, dtype=jnp.int32)
    causal = positions[None, :] < positions[:, None]
    start_log = jnp.zeros((local_heads, block_len), jnp.float32)
    totals, carry_log = piece_terms(
        queries,
        key_flat.reshape(block_len, local_heads, HD),
        value_flat.reshape(block_len, local_heads, HD),
        key_offset,
        start_log,
        causal,
    )

    def visit(hop_count, carried):
        running, running_log, moving = carried
        moving = shifted((moving[0], moving[1], moving[2]), "sp", 1)
        result, next_log = piece_terms(
            queries,
            moving[0].reshape(block_len, local_heads, HD),
            moving[1].reshape(block_len, local_heads, HD),
            moving[2],
            running_log,
            None,
        )
        active = position >= hop_count
        running = jnp.where(active, running + result, running)
        running_log = jnp.where(active, next_log, running_log)
        return (running, running_log, moving)

    totals, carry_log, leftover = lax.fori_loop(
        1, lax.axis_size("sp"), visit, (totals, carry_log, (key_flat, value_flat, key_offset))
    )
    attn_heads = totals.reshape(block_len, head_cols).astype(jnp.bfloat16)
    gated_input = (
        conv_value.astype(jnp.float32) * jax.nn.sigmoid(conv_gate.astype(jnp.float32))
    ).astype(jnp.bfloat16)
    kernel_len = conv_kernel.shape[0]
    edge_rows = shifted(gated_input[block_len - (kernel_len - 1) :], "sp", 1)
    extended = jnp.concatenate([edge_rows, gated_input], axis=0).astype(jnp.float32)
    conv_sum = jnp.zeros((block_len, channels), jnp.float32)
    for tap_index in range(kernel_len):
        conv_sum = conv_sum + conv_kernel[tap_index] * extended[tap_index : tap_index + block_len]
    channel_total = lax.psum(jnp.sum(conv_sum, axis=1), "tp")
    centred = conv_sum - (channel_total / CC)[:, None]
    spread = lax.psum(jnp.sum(centred * centred, axis=1), "tp") / CC
    conv_hidden = jax.nn.silu(centred * lax.rsqrt(spread + 1e-06)[:, None] * conv_gain).astype(
        jnp.bfloat16
    )
    attn_weight, conv_weight = (
        lax.all_gather(w_attn_out, "fs", axis=1, tiled=True),
        lax.all_gather(w_conv_out, "fs", axis=1, tiled=True),
    )
    partial_value = jnp.dot(attn_heads, attn_weight, preferred_element_type=jnp.float32)
    partial_value = partial_value + jnp.dot(
        conv_hidden, conv_weight, preferred_element_type=jnp.float32
    )
    mixed = lax.psum_scatter(
        lax.optimization_barrier(partial_value.astype(jnp.bfloat16))
        .astype(jnp.float32)
        .astype(jnp.bfloat16),
        "tp",
        scatter_dimension=0,
        tiled=True,
    )
    return mixed[None]

def xor_perm(block, axis, bit):
    return lax.ppermute(block, axis, [(i, i ^ bit) for i in range(lax.axis_size(axis))])


def turned(block, axis, distance):
    count = lax.axis_size(axis)
    return lax.ppermute(block, axis, [(i, (i + distance) % count) for i in range(count)])


def square_gather(block):
    half = block.shape[0] // 2
    first = xor_perm(block, "fs", 1)
    second = xor_perm(block, "fs", 2)
    upper = xor_perm(second[:half], "fs", 1)
    lower = xor_perm(first[half:], "fs", 2)
    return [block, first, second, upper, lower]


def whole_spec(shape):
    return pl.BlockSpec(shape, lambda: (0,) * len(shape), memory_space=pltpu.VMEM)


def call(body, place, operands, outs, scratch=(), flops=0, name=None):
    return pl.pallas_call(
        body,
        in_specs=[pl.BlockSpec(memory_space=pltpu.SMEM)] + [whole_spec(x.shape) for x in operands],
        out_specs=[whole_spec(x.shape) for x in outs],
        out_shape=list(outs),
        scratch_shapes=list(scratch),
        compiler_params=pltpu.CompilerParams(vmem_limit_bytes=56 * 2**20),
        cost_estimate=pl.CostEstimate(flops=flops, transcendentals=0, bytes_accessed=0),
        name=name,
    )(place, *operands)


def square_pieces(refs):
    half = refs[3].shape[0]
    return [(0, 0, refs[0]), (1, 0, refs[1]), (2, 0, refs[2]), (3, 0, refs[3]), (3, half, refs[4])]


def project_kernel(count, place, *refs):
    own, other, weights, out = refs[:count], refs[count : 2 * count], refs[2 * count : -1], refs[-1]
    rows, part = own[0].shape[0], weights[0].shape[0]
    sp, tp, fs = place[0], place[1], place[2]
    for d in range(count):
        total = None
        for bit, start, weight in square_pieces(weights):
            first = pl.multiple_of((fs ^ bit) * part + start, 128)
            cols = pl.ds(first, weight.shape[0])
            left = jnp.concatenate([own[d][:, cols], other[d][:, cols]], axis=0)
            term = jnp.dot(left, weight[...], preferred_element_type=jnp.float32)
            total = term if total is None else total + term
        total = total.astype(jnp.bfloat16)
        block = lax.rem(sp - d + count, count) * 2
        out[pl.ds(pl.multiple_of((block + tp) * rows, rows), rows), :] = total[:rows]
        out[pl.ds(pl.multiple_of((block + 1 - tp) * rows, rows), rows), :] = total[rows:]


def conv_kernel_body(count, place, projected, taps, out, padded):
    length, width = projected.shape[0], taps.shape[1]
    tap_count = taps.shape[0]
    front = padded.shape[0] - length
    first = projected.shape[1] - 2 * width
    padded[:front] = jnp.zeros((front, width), jnp.float32)
    step = 128
    for row in range(0, length, step):
        value = projected[row : row + step, first : first + width].astype(jnp.float32)
        gate = projected[row : row + step, first + width :].astype(jnp.float32)
        gated = (value * jax.nn.sigmoid(gate)).astype(jnp.bfloat16)
        padded[front + row : front + row + step] = gated.astype(jnp.float32)
    block_len = length // count
    for row in range(0, length, step):
        total = jnp.zeros((step, width), jnp.float32)
        for tap in range(tap_count):
            start = front + row - (tap_count - 1) + tap
            total = total + taps[tap : tap + 1, :] * padded[start : start + step, :]
        slot = lax.rem(row // block_len - place[0] + count, count)
        target = pl.multiple_of(slot * block_len + row % block_len, step)
        out[pl.ds(target, step), :] = total


def attention_kernel(count, heads, place, projected, offsets, out):
    length = projected.shape[0]
    width = heads * HD
    block = length // count
    row_index = lax.broadcasted_iota(jnp.int32, (block, block), 0)
    col_index = lax.broadcasted_iota(jnp.int32, (block, block), 1)
    allowed = col_index < row_index
    suffix = (row_index >= col_index).astype(jnp.bfloat16)
    for i in range(count):
        results = []
        for h in range(heads):
            query = projected[i * block : (i + 1) * block, h * HD : (h + 1) * HD]
            carry = None
            total = None
            for j in range(i, -1, -1):
                rows = slice(j * block, (j + 1) * block)
                key = projected[rows, width + h * HD : width + (h + 1) * HD]
                value = projected[rows, 2 * width + h * HD : 2 * width + (h + 1) * HD]
                logits = lax.dot_general(
                    query, key, (((1,), (1,)), ((), ())), preferred_element_type=jnp.float32
                ) * HD ** (-0.5)
                logits = logits + offsets[h : h + 1, rows]
                log_keep = jnp.minimum(-logits, 0.0) - jnp.log(1.0 + jnp.exp(-jnp.abs(logits)))
                if i == j:
                    log_keep = jnp.where(allowed, log_keep, 0.0)
                high = log_keep.astype(jnp.bfloat16)
                low = (log_keep - high.astype(jnp.float32)).astype(jnp.bfloat16)
                summed = jnp.dot(high, suffix, preferred_element_type=jnp.float32) + jnp.dot(
                    low, suffix, preferred_element_type=jnp.float32
                )
                if carry is not None:
                    summed = summed + carry
                weights = jnp.exp(logits + summed)
                if i == j:
                    weights = jnp.where(allowed, weights, 0.0)
                carry = summed[:, :1]
                term = jnp.dot(
                    weights.astype(jnp.bfloat16), value, preferred_element_type=jnp.float32
                )
                total = term if total is None else total + term
            results.append(total.astype(jnp.bfloat16))
        slot = lax.rem(i - place[0] + count, count)
        out[pl.ds(pl.multiple_of(slot * block, block), block), :] = jnp.concatenate(results, axis=1)


def stats_kernel(count, place, *refs):
    parts, out, stats = refs[:count], refs[count], refs[count + 1]
    width = parts[0].shape[1]
    total = sum(jnp.sum(part[...], axis=1, keepdims=True) for part in parts)
    mean = total / (count * width)
    spread = 0.0
    for d in range(count):
        centred = parts[d][...] - mean
        spread = spread + jnp.sum(centred * centred, axis=1, keepdims=True)
        channel = lax.rem(place[0] - d + count, count)
        out[:, pl.ds(pl.multiple_of(channel * width, width), width)] = centred
    lane = lax.broadcasted_iota(jnp.int32, stats.shape, 1)
    stats[...] = jnp.where(lane == 0, mean, jnp.where(lane == 1, spread, 0.0))


def output_kernel(count, place, *refs):
    heads = refs[:count]
    centred, stats, far_stats, gain = refs[count : count + 4]
    attn_weights = refs[count + 4 : count + 9]
    conv_weights = refs[count + 9 : count + 14]
    keep, send, attn, hidden = refs[count + 14 :]
    sp, tp, fs = place[0], place[1], place[2]
    width = heads[0].shape[1]
    rows = keep.shape[0]
    own_rows = pl.ds(pl.multiple_of(tp * rows, rows), rows)
    far_rows = pl.ds(pl.multiple_of((1 - tp) * rows, rows), rows)
    for d in range(count):
        channel = lax.rem(sp - d + count, count)
        cols = pl.ds(pl.multiple_of(channel * width, width), width)
        attn[:rows, cols] = heads[d][own_rows, :]
        attn[rows:, cols] = heads[d][far_rows, :]
    channels = centred.shape[1]
    for source, target in ((own_rows, slice(0, rows)), (far_rows, slice(rows, None))):
        mean, spread = stats[source, 0:1], stats[source, 1:2]
        far_mean, far_spread = far_stats[source, 0:1], far_stats[source, 1:2]
        shift = 0.5 * (mean - far_mean)
        variance = (spread + far_spread + 2 * channels * shift * shift) / (2 * channels)
        scaled = (centred[source, :] + shift) * lax.rsqrt(variance + 1e-06) * gain[...]
        hidden[target, :] = jax.nn.silu(scaled).astype(jnp.bfloat16)
    cols = attn_weights[0].shape[1]
    half = attn_weights[3].shape[0]
    for bit in range(4):
        picked = pl.ds(pl.multiple_of((fs ^ bit) * cols, cols), cols)
        if bit < 3:
            total = jnp.dot(attn[...], attn_weights[bit][...], preferred_element_type=jnp.float32)
            total = total + jnp.dot(
                hidden[...], conv_weights[bit][...], preferred_element_type=jnp.float32
            )
        else:
            total = 0.0
            for left, weights in ((attn, attn_weights), (hidden, conv_weights)):
                for start, weight in ((0, weights[3]), (half, weights[4])):
                    total = total + jnp.dot(
                        left[:, start : start + half],
                        weight[...],
                        preferred_element_type=jnp.float32,
                    )
        total = total.astype(jnp.bfloat16)
        keep[:, picked] = total[:rows]
        send[:, picked] = total[rows:]


def split_shards(
    tokens,
    norm_gain,
    w_query,
    w_key,
    w_value,
    w_conv_value,
    w_conv_gate,
    key_offset,
    conv_kernel,
    conv_gain,
    w_attn_out,
    w_conv_out,
):
    count = lax.axis_size("sp")
    sp, tp, fs = lax.axis_index("sp"), lax.axis_index("tp"), lax.axis_index("fs")
    place = jnp.stack([sp, tp, fs]).astype(jnp.int32)
    width = w_query.shape[1] // count
    heads = width // HD
    rows = tokens.shape[1]
    block = 2 * rows
    length = block * count

    floats = tokens[0].astype(jnp.float32)
    normed = (
        floats * lax.rsqrt(jnp.mean(floats * floats, axis=1, keepdims=True) + 1e-06) * norm_gain
    ).astype(jnp.bfloat16)
    own = [normed] + [turned(normed, "sp", d) for d in range(1, count)]
    offsets = [key_offset] + [turned(key_offset, "sp", d) for d in range(1, count)]
    other = [xor_perm(chunk, "tp", 1) for chunk in own]

    columns = jnp.concatenate(
        [
            lax.dynamic_slice_in_dim(weight, sp * width, width, 1)
            for weight in (w_query, w_key, w_value, w_conv_value, w_conv_gate)
        ],
        axis=1,
    )
    in_weights = square_gather(columns)
    attn_out, conv_out, in_weights = lax.optimization_barrier((w_attn_out, w_conv_out, in_weights))
    attn_weights = square_gather(attn_out)
    conv_weights = square_gather(conv_out)

    total_cols = columns.shape[1]
    (projected,) = call(
        functools.partial(project_kernel, count),
        place,
        own + other + in_weights,
        [jax.ShapeDtypeStruct((length, total_cols), jnp.bfloat16)],
        flops=2 * length * total_cols * tokens.shape[2],
        name="project",
    )
    own_taps = lax.dynamic_slice_in_dim(conv_kernel, sp * width, width, 1)
    tap_pad = -(-(conv_kernel.shape[0] - 1) // 8) * 8
    (conv_sum,) = call(
        functools.partial(conv_kernel_body, count),
        place,
        [projected, own_taps],
        [jax.ShapeDtypeStruct((length, width), jnp.float32)],
        [pltpu.VMEM((length + tap_pad, width), jnp.float32)],
        flops=10**8,
        name="conv",
    )
    conv_parts = [conv_sum[:block]] + [
        turned(conv_sum[d * block : (d + 1) * block], "sp", d) for d in range(1, count)
    ]

    stacked = jnp.zeros((count,) + key_offset.shape, key_offset.dtype)
    for d in range(count):
        stacked = lax.dynamic_update_slice_in_dim(
            stacked, offsets[d][None], lax.rem(sp - d + count, count), 0
        )
    own_offsets = lax.dynamic_slice_in_dim(
        stacked.reshape(length, key_offset.shape[1]), sp * heads, heads, 1
    )
    own_offsets = jnp.transpose(own_offsets.astype(jnp.float32))
    (attn_all,) = call(
        functools.partial(attention_kernel, count, heads),
        place,
        [projected, own_offsets],
        [jax.ShapeDtypeStruct((length, width), jnp.bfloat16)],
        flops=10**10,
        name="attention",
    )
    head_parts = [attn_all[:block]] + [
        turned(attn_all[d * block : (d + 1) * block], "sp", d) for d in range(1, count)
    ]
    centred, stats = call(
        functools.partial(stats_kernel, count),
        place,
        conv_parts,
        [
            jax.ShapeDtypeStruct((block, width * count), jnp.float32),
            jax.ShapeDtypeStruct((block, 128), jnp.float32),
        ],
        flops=10**7,
        name="stats",
    )
    far_stats = xor_perm(stats, "tp", 1)
    model = w_attn_out.shape[1] * lax.axis_size("fs")
    keep, send = call(
        functools.partial(output_kernel, count),
        place,
        head_parts + [centred, stats, far_stats, conv_gain[None]] + attn_weights + conv_weights,
        [jax.ShapeDtypeStruct((rows, model), jnp.bfloat16)] * 2,
        [
            pltpu.VMEM((block, width * count), jnp.bfloat16),
            pltpu.VMEM((block, width * count), jnp.bfloat16),
        ],
        flops=4 * block * width * count * model,
        name="output",
    )
    received = xor_perm(send, "tp", 1)
    mixed = (keep.astype(jnp.float32) + received.astype(jnp.float32)).astype(jnp.bfloat16)
    return mixed[None]


def solution(mesh):
    placed = (
        P("fs", ("sp", "tp"), None),
        P(),
        P("fs", "tp"),
        P("fs", "tp"),
        P("fs", "tp"),
        P("fs", "tp"),
        P("fs", "tp"),
        P("sp", "tp"),
        P(None, "tp"),
        P("tp"),
        P("tp", "fs"),
        P("tp", "fs"),
    )

    def chosen(*args):
        head_cols, channels = args[2].shape[1], args[5].shape[1]
        splits = head_cols == channels and head_cols % (mesh.shape["sp"] * 128) == 0
        if splits and mesh.shape["fs"] == 4 and mesh.shape["tp"] == 2:
            return split_shards(*args)
        return shards(*args)

    return jax.shard_map(
        chosen, mesh=mesh, in_specs=placed, out_specs=P("fs", ("sp", "tp"), None), check_vma=False
    )
```

```python
import functools

import jax
import jax.numpy as jnp
from jax import lax
from jax.experimental import pallas as pl
from jax.experimental.pallas import tpu as pltpu
from jax.sharding import PartitionSpec as P

HD = 64
CC = 1024


def shifted(block, axis, distance):
    devices = range(lax.axis_size(axis))
    route = [(i - distance, i) for i in devices if i - distance in devices]
    return lax.ppermute(block, axis, route)


def piece_terms(queries, key_rows, value_rows, offsets, carry_log, allowed):
    head_size = queries.shape[2]
    logits = jnp.einsum(
        "qhd,khd->hqk", queries, key_rows, preferred_element_type=jnp.float32
    ) * head_size ** (-0.5)
    logits = logits + jnp.transpose(offsets.astype(jnp.float32))[:, None, :]
    log_keep = jax.nn.log_sigmoid(-logits)
    if allowed is not None:
        log_keep = jnp.where(allowed[None], log_keep, 0.0)
    between = lax.cumsum(log_keep, axis=2, reverse=True) - log_keep
    weights = jnp.exp(jax.nn.log_sigmoid(logits) + between + carry_log[:, :, None])
    if allowed is not None:
        weights = jnp.where(allowed[None], weights, 0.0)
    result = jnp.einsum(
        "hqk,khd->qhd", weights.astype(jnp.bfloat16), value_rows, preferred_element_type=jnp.float32
    )
    return (result, carry_log + jnp.sum(log_keep, axis=2))


def shards(
    tokens,
    norm_gain,
    w_query,
    w_key,
    w_value,
    w_conv_value,
    w_conv_gate,
    key_offset,
    conv_kernel,
    conv_gain,
    w_attn_out,
    w_conv_out,
):
    gathered = (
        lax.all_gather(w_query, "fs", axis=0, tiled=True),
        lax.all_gather(w_key, "fs", axis=0, tiled=True),
        lax.all_gather(w_value, "fs", axis=0, tiled=True),
        lax.all_gather(w_conv_value, "fs", axis=0, tiled=True),
        lax.all_gather(w_conv_gate, "fs", axis=0, tiled=True),
    )
    floats = lax.all_gather(tokens[0], "tp", axis=0, tiled=True).astype(jnp.float32)
    normed = (
        floats * lax.rsqrt(jnp.mean(floats * floats, axis=1, keepdims=True) + 1e-06) * norm_gain
    ).astype(jnp.bfloat16)
    projected = jnp.concatenate(
        [
            jnp.dot(normed, weight, preferred_element_type=jnp.float32).astype(jnp.bfloat16)
            for weight in gathered
        ],
        axis=1,
    )
    head_cols = w_query.shape[1]
    channels = w_conv_value.shape[1]
    block_len = projected.shape[0]
    local_heads = head_cols // HD
    queries = projected[:, :head_cols].reshape(block_len, local_heads, HD)
    key_flat = projected[:, head_cols : 2 * head_cols]
    value_flat = projected[:, 2 * head_cols : 3 * head_cols]
    conv_value = projected[:, 3 * head_cols : 3 * head_cols + channels]
    conv_gate = projected[:, 3 * head_cols + channels :]
    position = lax.axis_index("sp")
    positions = jnp.arange(block_len, dtype=jnp.int32)
    causal = positions[None, :] < positions[:, None]
    start_log = jnp.zeros((local_heads, block_len), jnp.float32)
    totals, carry_log = piece_terms(
        queries,
        key_flat.reshape(block_len, local_heads, HD),
        value_flat.reshape(block_len, local_heads, HD),
        key_offset,
        start_log,
        causal,
    )

    def visit(hop_count, carried):
        running, running_log, moving = carried
        moving = shifted((moving[0], moving[1], moving[2]), "sp", 1)
        result, next_log = piece_terms(
            queries,
            moving[0].reshape(block_len, local_heads, HD),
            moving[1].reshape(block_len, local_heads, HD),
            moving[2],
            running_log,
            None,
        )
        active = position >= hop_count
        running = jnp.where(active, running + result, running)
        running_log = jnp.where(active, next_log, running_log)
        return (running, running_log, moving)

    totals, carry_log, leftover = lax.fori_loop(
        1, lax.axis_size("sp"), visit, (totals, carry_log, (key_flat, value_flat, key_offset))
    )
    attn_heads = totals.reshape(block_len, head_cols).astype(jnp.bfloat16)
    gated_input = (
        conv_value.astype(jnp.float32) * jax.nn.sigmoid(conv_gate.astype(jnp.float32))
    ).astype(jnp.bfloat16)
    kernel_len = conv_kernel.shape[0]
    edge_rows = shifted(gated_input[block_len - (kernel_len - 1) :], "sp", 1)
    extended = jnp.concatenate([edge_rows, gated_input], axis=0).astype(jnp.float32)
    conv_sum = jnp.zeros((block_len, channels), jnp.float32)
    for tap_index in range(kernel_len):
        conv_sum = conv_sum + conv_kernel[tap_index] * extended[tap_index : tap_index + block_len]
    channel_total = lax.psum(jnp.sum(conv_sum, axis=1), "tp")
    centred = conv_sum - (channel_total / CC)[:, None]
    spread = lax.psum(jnp.sum(centred * centred, axis=1), "tp") / CC
    conv_hidden = jax.nn.silu(centred * lax.rsqrt(spread + 1e-06)[:, None] * conv_gain).astype(
        jnp.bfloat16
    )
    attn_weight, conv_weight = (
        lax.all_gather(w_attn_out, "fs", axis=1, tiled=True),
        lax.all_gather(w_conv_out, "fs", axis=1, tiled=True),
    )
    partial_value = jnp.dot(attn_heads, attn_weight, preferred_element_type=jnp.float32)
    partial_value = partial_value + jnp.dot(
        conv_hidden, conv_weight, preferred_element_type=jnp.float32
    )
    mixed = lax.psum_scatter(
        lax.optimization_barrier(partial_value.astype(jnp.bfloat16))
        .astype(jnp.float32)
        .astype(jnp.bfloat16),
        "tp",
        scatter_dimension=0,
        tiled=True,
    )
    return mixed[None]

def xor_perm(block, axis, bit):
    return lax.ppermute(block, axis, [(i, i ^ bit) for i in range(lax.axis_size(axis))])


def turned(block, axis, distance):
    count = lax.axis_size(axis)
    return lax.ppermute(block, axis, [(i, (i + distance) % count) for i in range(count)])


def square_sides(block):
    return [block, xor_perm(block, "fs", 1), xor_perm(block, "fs", 2)]


def square_rest(sides):
    half = sides[0].shape[0] // 2
    upper = xor_perm(sides[2][:half], "fs", 1)
    lower = xor_perm(sides[1][half:], "fs", 2)
    return sides + [upper, lower]


def whole_spec(shape):
    return pl.BlockSpec(shape, lambda: (0,) * len(shape), memory_space=pltpu.VMEM)


def call(
    body, place, operands, outs, scratch=(), flops=0, name=None, far=()
):
    hbm = pl.BlockSpec(memory_space=pl.ANY)
    return pl.pallas_call(
        body,
        in_specs=[pl.BlockSpec(memory_space=pltpu.SMEM)]
        + [hbm if i in far else whole_spec(x.shape) for i, x in enumerate(operands)],
        out_specs=[whole_spec(x.shape) for x in outs],
        out_shape=list(outs),
        scratch_shapes=list(scratch),
        compiler_params=pltpu.CompilerParams(vmem_limit_bytes=56 * 2**20),
        cost_estimate=pl.CostEstimate(flops=flops, transcendentals=0, bytes_accessed=0),
        name=name,
    )(place, *operands)


def columns_kernel(place, *refs):
    count = len(refs) - 2
    weights, out, sems = refs[:count], refs[count], refs[count + 1]
    width = out.shape[1] // count
    first = pl.multiple_of(place[0] * width, width)
    copies = [
        pltpu.make_async_copy(
            weight.at[:, pl.ds(first, width)],
            out.at[:, k * width : (k + 1) * width],
            sems.at[k],
        )
        for k, weight in enumerate(weights)
    ]
    for copy in copies:
        copy.start()
    for copy in copies:
        copy.wait()


def square_pieces(refs):
    half = refs[3].shape[0]
    return [(0, 0, refs[0]), (1, 0, refs[1]), (2, 0, refs[2]), (3, 0, refs[3]), (3, half, refs[4])]


def project_rows(place, own, other, weights, result):
    rows, part = own.shape[0], weights[0].shape[0]
    tp, fs = place[1], place[2]
    total = None
    for bit, start, weight in square_pieces(weights):
        first = pl.multiple_of((fs ^ bit) * part + start, 128)
        cols = pl.ds(first, weight.shape[0])
        left = jnp.concatenate([own[:, cols], other[:, cols]], axis=0)
        term = jnp.dot(left, weight[...], preferred_element_type=jnp.float32)
        total = term if total is None else total + term
    total = total.astype(jnp.bfloat16)
    result[pl.ds(pl.multiple_of(tp * rows, rows), rows), :] = total[:rows]
    result[pl.ds(pl.multiple_of((1 - tp) * rows, rows), rows), :] = total[rows:]


def project_kernel(count, place, *refs):
    own, own_other, twice, twice_other, left, left_other, right, right_other = refs[:8]
    last, last_other = refs[8:10]
    weights, out = refs[10:15], refs[15]
    sp = place[0]
    rows = 2 * own.shape[0]

    def target(distance):
        block = lax.rem(sp + distance, count)
        return out.at[pl.ds(pl.multiple_of(block * rows, rows), rows)]

    project_rows(place, own, own_other, weights, target(0))
    project_rows(place, twice, twice_other, weights, target(2))

    @pl.when(sp > 0)
    def _():
        project_rows(place, left, left_other, weights, target(count - 1))

    @pl.when(sp < count - 1)
    def _():
        project_rows(place, right, right_other, weights, target(1))

    @pl.when(sp == 0)
    def _():
        project_rows(place, last, last_other, weights, target(count - 1))

    @pl.when(sp == count - 1)
    def _():
        project_rows(place, last, last_other, weights, target(1))


def conv_kernel_body(count, place, projected, taps, *refs):
    outs, padded, sums = refs[:count], refs[count], refs[count + 1]
    length, width = projected.shape[0], taps.shape[1]
    tap_count = taps.shape[0]
    front = padded.shape[0] - length
    first = projected.shape[1] - 2 * width
    padded[:front] = jnp.zeros((front, width), jnp.float32)
    step = 128
    for row in range(0, length, step):
        value = projected[row : row + step, first : first + width].astype(jnp.float32)
        gate = projected[row : row + step, first + width :].astype(jnp.float32)
        gated = (value * jax.nn.sigmoid(gate)).astype(jnp.bfloat16)
        padded[front + row : front + row + step] = gated.astype(jnp.float32)
    block_len = length // count
    for row in range(0, length, step):
        total = jnp.zeros((step, width), jnp.float32)
        for tap in range(tap_count):
            start = front + row - (tap_count - 1) + tap
            total = total + taps[tap : tap + 1, :] * padded[start : start + step, :]
        sums[row : row + step] = total
    turn_out(count, place, sums, outs)


def turn_out(count, place, whole, outs):
    rows = outs[0].shape[0]
    for d in range(count):
        block = lax.rem(place[0] + d, count)
        outs[d][...] = whole[pl.ds(pl.multiple_of(block * rows, rows), rows), :]


def attention_kernel(count, heads, place, projected, offsets, *refs):
    outs, found = refs[:count], refs[count]
    length = projected.shape[0]
    width = heads * HD
    block = length // count
    row_index = lax.broadcasted_iota(jnp.int32, (block, block), 0)
    col_index = lax.broadcasted_iota(jnp.int32, (block, block), 1)
    allowed = col_index < row_index
    suffix = (row_index >= col_index).astype(jnp.bfloat16)
    for i in range(count):
        results = []
        for h in range(heads):
            query = projected[i * block : (i + 1) * block, h * HD : (h + 1) * HD]
            carry = None
            total = None
            for j in range(i, -1, -1):
                rows = slice(j * block, (j + 1) * block)
                key = projected[rows, width + h * HD : width + (h + 1) * HD]
                value = projected[rows, 2 * width + h * HD : 2 * width + (h + 1) * HD]
                logits = lax.dot_general(
                    query, key, (((1,), (1,)), ((), ())), preferred_element_type=jnp.float32
                ) * HD ** (-0.5)
                logits = logits + offsets[h : h + 1, rows]
                log_keep = jnp.minimum(-logits, 0.0) - jnp.log(1.0 + jnp.exp(-jnp.abs(logits)))
                if i == j:
                    log_keep = jnp.where(allowed, log_keep, 0.0)
                high = log_keep.astype(jnp.bfloat16)
                low = (log_keep - high.astype(jnp.float32)).astype(jnp.bfloat16)
                summed = jnp.dot(high, suffix, preferred_element_type=jnp.float32) + jnp.dot(
                    low, suffix, preferred_element_type=jnp.float32
                )
                if carry is not None:
                    summed = summed + carry
                weights = jnp.exp(logits + summed)
                if i == j:
                    weights = jnp.where(allowed, weights, 0.0)
                carry = summed[:, :1]
                term = jnp.dot(
                    weights.astype(jnp.bfloat16), value, preferred_element_type=jnp.float32
                )
                total = term if total is None else total + term
            results.append(total.astype(jnp.bfloat16))
        found[i * block : (i + 1) * block] = jnp.concatenate(results, axis=1)
    turn_out(count, place, found, outs)


def stats_kernel(count, place, *refs):
    parts, out, stats = refs[:count], refs[count], refs[count + 1]
    width = parts[0].shape[1]
    total = sum(jnp.sum(part[...], axis=1, keepdims=True) for part in parts)
    mean = total / (count * width)
    spread = 0.0
    for d in range(count):
        centred = parts[d][...] - mean
        spread = spread + jnp.sum(centred * centred, axis=1, keepdims=True)
        channel = lax.rem(place[0] - d + count, count)
        out[:, pl.ds(pl.multiple_of(channel * width, width), width)] = centred
    lane = lax.broadcasted_iota(jnp.int32, stats.shape, 1)
    stats[...] = jnp.where(lane == 0, mean, jnp.where(lane == 1, spread, 0.0))


def output_kernel(count, place, *refs):
    heads = refs[:count]
    centred, stats, far_stats, gain = refs[count : count + 4]
    attn_weights = refs[count + 4 : count + 9]
    conv_weights = refs[count + 9 : count + 14]
    keep, send, attn, hidden = refs[count + 14 :]
    sp, tp, fs = place[0], place[1], place[2]
    width = heads[0].shape[1]
    rows = keep.shape[0]
    own_rows = pl.ds(pl.multiple_of(tp * rows, rows), rows)
    far_rows = pl.ds(pl.multiple_of((1 - tp) * rows, rows), rows)
    for d in range(count):
        channel = lax.rem(sp - d + count, count)
        cols = pl.ds(pl.multiple_of(channel * width, width), width)
        attn[:rows, cols] = heads[d][own_rows, :]
        attn[rows:, cols] = heads[d][far_rows, :]
    channels = centred.shape[1]
    for source, target in ((own_rows, slice(0, rows)), (far_rows, slice(rows, None))):
        mean, spread = stats[source, 0:1], stats[source, 1:2]
        far_mean, far_spread = far_stats[source, 0:1], far_stats[source, 1:2]
        shift = 0.5 * (mean - far_mean)
        variance = (spread + far_spread + 2 * channels * shift * shift) / (2 * channels)
        scaled = (centred[source, :] + shift) * lax.rsqrt(variance + 1e-06) * gain[...]
        hidden[target, :] = jax.nn.silu(scaled).astype(jnp.bfloat16)
    cols = attn_weights[0].shape[1]
    half = attn_weights[3].shape[0]
    for bit in range(4):
        picked = pl.ds(pl.multiple_of((fs ^ bit) * cols, cols), cols)
        if bit < 3:
            total = jnp.dot(attn[...], attn_weights[bit][...], preferred_element_type=jnp.float32)
            total = total + jnp.dot(
                hidden[...], conv_weights[bit][...], preferred_element_type=jnp.float32
            )
        else:
            total = 0.0
            for left, weights in ((attn, attn_weights), (hidden, conv_weights)):
                for start, weight in ((0, weights[3]), (half, weights[4])):
                    total = total + jnp.dot(
                        left[:, start : start + half],
                        weight[...],
                        preferred_element_type=jnp.float32,
                    )
        total = total.astype(jnp.bfloat16)
        keep[:, picked] = total[:rows]
        send[:, picked] = total[rows:]


def split_shards(
    tokens,
    norm_gain,
    w_query,
    w_key,
    w_value,
    w_conv_value,
    w_conv_gate,
    key_offset,
    conv_kernel,
    conv_gain,
    w_attn_out,
    w_conv_out,
):
    count = lax.axis_size("sp")
    sp, tp, fs = lax.axis_index("sp"), lax.axis_index("tp"), lax.axis_index("fs")
    place = jnp.stack([sp, tp, fs]).astype(jnp.int32)
    width = w_query.shape[1] // count
    heads = width // HD
    rows = tokens.shape[1]
    block = 2 * rows
    length = block * count

    floats = tokens[0].astype(jnp.float32)
    normed = (
        floats * lax.rsqrt(jnp.mean(floats * floats, axis=1, keepdims=True) + 1e-06) * norm_gain
    ).astype(jnp.bfloat16)
    offsets = [key_offset] + [turned(key_offset, "sp", d) for d in range(1, count)]
    normed, offsets, w_query = lax.optimization_barrier((normed, offsets, w_query))
    twice = turned(normed, "sp", 2)
    left = shifted(normed, "sp", 1)
    right = lax.ppermute(normed, "sp", [(i + 1, i) for i in range(count - 1)])

    (columns,) = call(
        columns_kernel,
        place,
        [w_query, w_key, w_value, w_conv_value, w_conv_gate],
        [jax.ShapeDtypeStruct((w_query.shape[0], 5 * width), jnp.bfloat16)],
        [pltpu.SemaphoreType.DMA((5,))],
        flops=10**6,
        name="columns",
        far=range(5),
    )
    in_weights = square_rest(square_sides(columns))
    twice, attn_out, conv_out, in_weights = lax.optimization_barrier(
        (twice, w_attn_out, w_conv_out, in_weights)
    )
    last = lax.ppermute(twice, "sp", [(count - 2, count - 1), (1, 0)])
    attn_weights = square_sides(attn_out)
    conv_weights = square_sides(conv_out)

    total_cols = columns.shape[1]
    chunks = []
    for chunk in (normed, twice, left, right, last):
        chunks += [chunk, xor_perm(chunk, "tp", 1)]
    chunks, attn_weights, conv_weights = lax.optimization_barrier(
        (chunks, attn_weights, conv_weights)
    )
    attn_weights, conv_weights = square_rest(attn_weights), square_rest(conv_weights)
    (projected,) = call(
        functools.partial(project_kernel, count),
        place,
        chunks + in_weights,
        [jax.ShapeDtypeStruct((length, total_cols), jnp.bfloat16)],
        flops=2 * length * total_cols * tokens.shape[2],
        name="project",
    )
    own_taps = lax.dynamic_slice_in_dim(conv_kernel, sp * width, width, 1)
    tap_pad = -(-(conv_kernel.shape[0] - 1) // 8) * 8
    conv_blocks = call(
        functools.partial(conv_kernel_body, count),
        place,
        [projected, own_taps],
        [jax.ShapeDtypeStruct((block, width), jnp.float32)] * count,
        [
            pltpu.VMEM((length + tap_pad, width), jnp.float32),
            pltpu.VMEM((length, width), jnp.float32),
        ],
        flops=10**8,
        name="conv",
    )
    conv_parts = [conv_blocks[0]] + [turned(conv_blocks[d], "sp", d) for d in range(1, count)]

    stacked = jnp.zeros((count,) + key_offset.shape, key_offset.dtype)
    for d in range(count):
        stacked = lax.dynamic_update_slice_in_dim(
            stacked, offsets[d][None], lax.rem(sp - d + count, count), 0
        )
    own_offsets = lax.dynamic_slice_in_dim(
        stacked.reshape(length, key_offset.shape[1]), sp * heads, heads, 1
    )
    own_offsets = jnp.transpose(own_offsets.astype(jnp.float32))
    head_blocks = call(
        functools.partial(attention_kernel, count, heads),
        place,
        [projected, own_offsets],
        [jax.ShapeDtypeStruct((block, width), jnp.bfloat16)] * count,
        [pltpu.VMEM((length, width), jnp.bfloat16)],
        flops=10**10,
        name="attention",
    )
    head_parts = [head_blocks[0]] + [turned(head_blocks[d], "sp", d) for d in range(1, count)]
    conv_parts, head_parts[0] = lax.optimization_barrier((conv_parts, head_parts[0]))
    centred, stats = call(
        functools.partial(stats_kernel, count),
        place,
        conv_parts,
        [
            jax.ShapeDtypeStruct((block, width * count), jnp.float32),
            jax.ShapeDtypeStruct((block, 128), jnp.float32),
        ],
        flops=10**7,
        name="stats",
    )
    far_stats = xor_perm(stats, "tp", 1)
    model = w_attn_out.shape[1] * lax.axis_size("fs")
    keep, send = call(
        functools.partial(output_kernel, count),
        place,
        head_parts + [centred, stats, far_stats, conv_gain[None]] + attn_weights + conv_weights,
        [jax.ShapeDtypeStruct((rows, model), jnp.bfloat16)] * 2,
        [
            pltpu.VMEM((block, width * count), jnp.bfloat16),
            pltpu.VMEM((block, width * count), jnp.bfloat16),
        ],
        flops=4 * block * width * count * model,
        name="output",
    )
    received = xor_perm(send, "tp", 1)
    mixed = (keep.astype(jnp.float32) + received.astype(jnp.float32)).astype(jnp.bfloat16)
    return mixed[None]


def solution(mesh):
    placed = (
        P("fs", ("sp", "tp"), None),
        P(),
        P("fs", "tp"),
        P("fs", "tp"),
        P("fs", "tp"),
        P("fs", "tp"),
        P("fs", "tp"),
        P("sp", "tp"),
        P(None, "tp"),
        P("tp"),
        P("tp", "fs"),
        P("tp", "fs"),
    )

    def chosen(*args):
        head_cols, channels = args[2].shape[1], args[5].shape[1]
        splits = head_cols == channels and head_cols % (mesh.shape["sp"] * 128) == 0
        if splits and mesh.shape["sp"] == mesh.shape["fs"] == 4 and mesh.shape["tp"] == 2:
            return split_shards(*args)
        return shards(*args)

    return jax.shard_map(
        chosen, mesh=mesh, in_specs=placed, out_specs=P("fs", ("sp", "tp"), None), check_vma=False
    )
```
